32 devices in a mesh: rep: 2 (over x), fs: 4 (over y, core), tp: 4 (over z).
Axes of the slice: x: 2, y: 2, z: 4, core: 2. Of those that a mesh axis runs over, the one named last changes fastest.
Arguments:
- inputs: bfloat16 [4096, 4096], P(('rep', 'fs', 'tp')), may hold values from -6 to 6
- w_gate: bfloat16 [4096, 11008], P('fs', 'tp'), may hold values from -0.09375 to 0.09375
- w_up: bfloat16 [4096, 11008], P('fs', 'tp'), may hold values from -0.09375 to 0.09375
- w_down: bfloat16 [11008, 4096], P('tp', 'fs'), may hold values from -0.0546875 to 0.0546875
- d_out: bfloat16 [4096, 4096], P(('rep', 'fs', 'tp')), may hold values from -6 to 6
Outputs:
- grad_inputs: bfloat16 [4096, 4096], P(('rep', 'fs', 'tp'))
- grad_gate: float32 [4096, 11008], P('fs', 'tp')
- grad_up: float32 [4096, 11008], P('fs', 'tp')
- grad_down: float32 [11008, 4096], P('tp', 'fs')
The draws below stay inside these ranges and needn't reach their ends.
All inputs are finite; a program needn't handle non-finite values.
Results may differ from the reference program's by a relative error of at most 0.00185.
Values may be sent and summed in bfloat16 or wider, within the bound.
A program may use at most 448 MiB of HBM per device.

```python
import jax
import jax.numpy as jnp
from jax import lax

D = 4096
FF = 11008
TOKENS = 4096


def raised(array, key, source, target, shards_of, factor):
    owner, partner = [(jnp.arange(array.shape[dim]) // (array.shape[dim] // shards_of)).reshape([-1 if axis == dim else 1 for axis in range(array.ndim)]) for dim in (source, target)]
    chosen = jax.random.permutation(key, shards_of)[partner]
    strong = (owner == chosen) | (owner == (partner + shards_of // 2) % shards_of)
    return jnp.where(strong, factor * array, array)


def shard_levels(key, extent, split, least, top_value):
    factor_of, own = 1.0, jax.random.fold_in(key, 6)
    for dim, blocks in split:
        heights = jnp.exp(jax.random.uniform(jax.random.fold_in(own, dim), (blocks,), jnp.float32, least / len(split), top_value / len(split)))
        factor_of = factor_of * jnp.repeat(heights, extent[dim] // blocks).reshape([-1 if axis == dim else 1 for axis in range(len(extent))])
    return factor_of


def centred(stream_key, dims, deviation, reach, pieces=(), kind=jnp.bfloat16):
    array = jax.random.normal(stream_key, dims, jnp.float32) * deviation
    if len(pieces) > 0:
        array = shard_levels(stream_key, dims, pieces, -0.22, 0.18) * array
    return jnp.clip(array, min=-reach, max=reach).astype(kind)


def bell_draw_with(key, extent, scale, reach, pieces, heavy, kind=jnp.bfloat16):
    drawn = scale * jax.random.normal(key, extent, jnp.float32)
    if pieces:
        drawn = drawn * shard_levels(key, extent, pieces, -0.22, 0.18)
    return jnp.clip(raised(drawn, jax.random.fold_in(key, 3), *heavy), -reach, reach).astype(kind)


def setup_inputs(seed: int = 0) -> dict:
    seeds = jax.random.split(jax.random.key(seed), 6)
    inputs = centred(seeds[0], (TOKENS, D), 1.0, 6.0, ((0, 32),))
    w_gate = centred(seeds[1], (D, FF), D ** -0.5, 0.09375, ((0, 4), (1, 4)))
    w_up = centred(seeds[2], (D, FF), D ** -0.5, 0.09375, ((0, 4), (1, 4)))
    w_down = centred(seeds[3], (FF, D), FF ** -0.5, 0.0546875, ((0, 4), (1, 4)))
    d_out = bell_draw_with(seeds[4], (TOKENS, D), 1.0, 6.0, ((0, 32),), (0, 1, 32, 2.75))
    return dict(inputs=inputs, w_gate=w_gate, w_up=w_up, w_down=w_down, d_out=d_out)


def stored(values):
    return lax.optimization_barrier(values.astype(jnp.bfloat16)).astype(jnp.float32)


def reference(inputs, w_gate, w_up, w_down, d_out):
    gate_val = stored(jnp.dot(inputs, w_gate, preferred_element_type=jnp.float32))
    up_val = stored(jnp.dot(inputs, w_up, preferred_element_type=jnp.float32))
    back_val = stored(jnp.dot(d_out, w_down.T, preferred_element_type=jnp.float32))
    sigma = jax.nn.sigmoid(gate_val)
    active = gate_val * sigma
    hidden = (active * up_val).astype(jnp.bfloat16)
    d_gate = (back_val * up_val * sigma * (1.0 + gate_val * (1.0 - sigma))).astype(jnp.bfloat16)
    d_up = (back_val * active).astype(jnp.bfloat16)
    grad_inputs = jnp.dot(d_gate, w_gate.T, preferred_element_type=jnp.float32)
    grad_inputs = grad_inputs + jnp.dot(d_up, w_up.T, preferred_element_type=jnp.float32)
    grad_inputs = grad_inputs.astype(jnp.bfloat16)
    grad_gate = jnp.dot(inputs.T, d_gate, preferred_element_type=jnp.float32)
    grad_up = jnp.dot(inputs.T, d_up, preferred_element_type=jnp.float32)
    grad_down = jnp.dot(hidden.T, d_out, preferred_element_type=jnp.float32)
    return grad_inputs, grad_gate, grad_up, grad_down
```

```python
import jax
import jax.numpy as jnp
from jax import lax
from jax.sharding import PartitionSpec as P


def stored(values):
    return lax.optimization_barrier(values.astype(jnp.bfloat16)).astype(jnp.float32)


def times_t(left, right):
    return lax.dot_general(
        left, right, (((1,), (1,)), ((), ())), preferred_element_type=jnp.float32
    )


def across_rows(left, right):
    return lax.dot_general(
        left, right, (((0,), (0,)), ((), ())), preferred_element_type=jnp.float32
    )


def whole_rows(shard):
    half = shard.shape[0] // lax.axis_size("rep")
    part = lax.dynamic_slice_in_dim(shard, lax.axis_index("rep") * half, half, 0)
    return lax.all_gather(part, ("fs", "rep"), axis=0, tiled=True)


def all_tokens(rows):
    return lax.all_gather(rows, ("rep", "fs"), axis=0, tiled=True)


def own_columns(shard):
    tokens = shard.shape[0]
    fs, tp, rep = lax.axis_size("fs"), lax.axis_size("tp"), lax.axis_size("rep")
    part = lax.all_to_all(shard, "fs", split_axis=1, concat_axis=0, tiled=True)
    part = lax.all_gather(part, ("rep", "tp"), axis=0, tiled=True)
    width = part.shape[1]
    part = part.reshape(rep, tp, fs, tokens, width).transpose(0, 2, 1, 3, 4)
    return part.reshape(rep * fs * tp * tokens, width)


def local(inputs, w_gate, w_up, w_down, d_out):
    rows_in = lax.all_gather(inputs, "tp", axis=0, tiled=True)
    full_gate = whole_rows(w_gate)
    full_up = whole_rows(w_up)
    rows_out = lax.all_gather(d_out, "tp", axis=0, tiled=True)
    full_down = whole_rows(w_down.T)
    gate_val = stored(jnp.dot(rows_in, full_gate, preferred_element_type=jnp.float32))
    up_val = stored(jnp.dot(rows_in, full_up, preferred_element_type=jnp.float32))
    sigma = jax.nn.sigmoid(gate_val)
    active = gate_val * sigma
    hidden = (active * up_val).astype(jnp.bfloat16)
    back_val = stored(jnp.dot(rows_out, full_down, preferred_element_type=jnp.float32))
    d_gate = (back_val * up_val * sigma * (1.0 + gate_val * (1.0 - sigma))).astype(jnp.bfloat16)
    d_up = (back_val * active).astype(jnp.bfloat16)

    cols_in = own_columns(inputs)
    cols_out = own_columns(d_out)
    grad_down = across_rows(all_tokens(hidden), cols_out)
    grad_gate = across_rows(cols_in, all_tokens(d_gate))
    grad_up = across_rows(cols_in, all_tokens(d_up))

    grad_inputs = times_t(d_gate, full_gate) + times_t(d_up, full_up)
    grad_inputs = lax.psum_scatter(grad_inputs, "tp", scatter_dimension=0, tiled=True)
    grad_inputs = grad_inputs.astype(jnp.bfloat16)
    return (grad_inputs, grad_gate, grad_up, grad_down)


def solution(mesh):
    return jax.shard_map(
        local,
        mesh=mesh,
        in_specs=(
            P(("rep", "fs", "tp"), None),
            P("fs", "tp"),
            P("fs", "tp"),
            P("tp", "fs"),
            P(("rep", "fs", "tp"), None),
        ),
        out_specs=(P(("rep", "fs", "tp"), None), P("fs", "tp"), P("fs", "tp"), P("tp", "fs")),
        check_vma=False,
    )
```
